32 devices in a mesh: grp: 2 (over y), fs: 4 (over z), tp: 4 (over x, core).
Axes of the slice: x: 2, y: 2, z: 4, core: 2. Of those that a mesh axis runs over, the one named last changes fastest.
Arguments:
- tokens: bfloat16 [6144, 2048], P(('grp', 'fs')), parts along dimension 0, may hold values from -6 to 6
- up_weight: bfloat16 [2048, 8192], P('fs', 'tp'), may hold values from -0.125 to 0.125
- down_weight: bfloat16 [8192, 2048], P('tp', 'fs'), may hold values from -0.0625 to 0.0625
- norm_gain: float32 [2048], replicated, may hold values from 0.1 to 1.9
- norm_shift: float32 [2048], replicated, may hold values from -3 to 3
Outputs:
- mixed: bfloat16 [6144, 2048], P(('grp', 'fs')), parts along dimension 0
The draws below stay inside these ranges and needn't reach their ends.
There are 2 independent parts, one for each index of `grp`. The reference program is written for one: setup_inputs(seed, part) draws one part's arguments, and reference() takes and returns one part's arrays. A program takes and returns all parts, laid end to end along the dimension named above; an argument that names none is the same for every part. Nothing has to cross between parts.
All inputs are finite; a program needn't handle non-finite values.
Results may differ from the reference program's by a relative error of at most 0.014.
Values may be sent and summed in bfloat16 or wider, within the bound.
A program may use at most 64 MiB of HBM per device.

```python
import jax
import jax.numpy as jnp
from jax import lax

D = 2048
FF = 8192
FF_DEV = 2048
TOKENS = 3072
N_TP = 4


def levels(own_key, extent, shards, low, high):
    def one(position, shards_of):
        heights = jax.random.uniform(jax.random.fold_in(jax.random.fold_in(own_key, 6), position), (shards_of,), jnp.float32, low / len(shards), high / len(shards))
        return jnp.repeat(jnp.exp(heights), extent[position] // shards_of).reshape((-1,) + (1,) * (len(extent) - position - 1))

    level = one(*shards[0])
    for cut in shards[1:]:
        level = level * one(*cut)
    return level


def noise(stream_key, extent, spread, bound, pieces=(), dtype=jnp.bfloat16):
    drawn = jax.random.normal(stream_key, extent, jnp.float32) * spread
    if len(pieces) > 0:
        drawn = levels(stream_key, extent, pieces, -0.22, 0.18) * drawn
    return jnp.clip(drawn, min=-bound, max=bound).astype(dtype)


def setup_inputs(seed: int = 0, part: int = 0) -> dict:
    arg_keys = jax.random.split(jax.random.key(seed), 6)
    part_keys = jax.random.split(jax.random.fold_in(arg_keys[5], part), 6)
    return {
        "tokens": noise(part_keys[0], (TOKENS, D), 1.0, 6.0, ((0, 4),)),
        "up_weight": noise(arg_keys[1], (D, FF), D ** -0.5, 0.125, ((0, 4), (1, 4))),
        "down_weight": noise(arg_keys[2], (FF, D), FF ** -0.5, 0.0625, ((0, 4), (1, 4))),
        "norm_gain": jnp.clip(1.0 + 0.18 * jax.random.normal(arg_keys[3], (D,), jnp.float32), 0.1, 1.9),
        "norm_shift": noise(arg_keys[4], (D,), 0.5, 3.0, (), jnp.float32),
    }


RESIDUAL_SCALE = 2.0 ** 0.25
NORM_EPS = 1e-05

def reference(tokens, up_weight, down_weight, norm_gain, norm_shift):
    upward = jnp.dot(tokens, up_weight, preferred_element_type=jnp.float32)
    hidden = jnp.square(jax.nn.relu(upward)).astype(jnp.bfloat16)
    row_total = hidden.shape[0]
    hidden_blocks = hidden.reshape(row_total, N_TP, FF_DEV).transpose(1, 0, 2)
    down_blocks = down_weight.reshape(N_TP, FF_DEV, D)

    def add_block(running, pair):
        partial_value = jnp.dot(pair[0], pair[1], preferred_element_type=jnp.float32).astype(jnp.bfloat16)
        partial_value = lax.optimization_barrier(partial_value)
        return (running + partial_value.astype(jnp.float32), None)
    summed, _ = lax.scan(add_block, jnp.zeros((row_total, D), jnp.float32), (hidden_blocks, down_blocks))
    pre_norm = RESIDUAL_SCALE * tokens.astype(jnp.float32) + summed
    centre = lax.optimization_barrier(jnp.mean(pre_norm, axis=-1, keepdims=True))
    centered = pre_norm - centre
    variance = lax.optimization_barrier(jnp.mean(centered * centered, axis=-1, keepdims=True))
    normed = centered * lax.rsqrt(variance + NORM_EPS) * norm_gain.astype(jnp.float32) + norm_shift.astype(jnp.float32)
    return normed.astype(jnp.bfloat16)
```

```python
import functools

import jax
import jax.numpy as jnp
from jax import lax
from jax.experimental import pallas as pl
from jax.experimental.pallas import tpu as pltpu
from jax.sharding import PartitionSpec as P

MESH = pl.DeviceIdType.MESH
RESIDUAL_SCALE = 2.0**0.25
NORM_EPS = 1e-05
SUBS = 4


def layer_normed(residual, summed, norm_gain, norm_shift):
    pre_norm = RESIDUAL_SCALE * residual.astype(jnp.float32) + summed
    centre = jnp.mean(pre_norm, axis=-1, keepdims=True)
    centered = pre_norm - centre
    variance = jnp.mean(centered * centered, axis=-1, keepdims=True)
    return (centered * lax.rsqrt(variance + NORM_EPS) * norm_gain + norm_shift).astype(jnp.bfloat16)


def general(tokens, up_weight, down_weight, norm_gain, norm_shift):
    upward = jnp.dot(
        tokens,
        lax.all_gather(up_weight, "fs", axis=0, tiled=True),
        preferred_element_type=jnp.float32,
    )
    down_full = lax.all_gather(down_weight, "fs", axis=1, tiled=True)
    hidden = jnp.square(jax.nn.relu(upward)).astype(jnp.bfloat16)
    share = tokens.shape[0] // lax.axis_size("tp")
    summed = lax.psum_scatter(
        jnp.dot(hidden, down_full, preferred_element_type=jnp.float32).astype(jnp.bfloat16),
        "tp",
        scatter_dimension=0,
        tiled=True,
    ).astype(jnp.float32)
    own_start = lax.axis_index("tp") * share
    own_tokens = lax.dynamic_slice_in_dim(tokens, own_start, share, 0)
    normed = layer_normed(own_tokens, summed, norm_gain, norm_shift)
    return lax.all_gather(normed, "tp", axis=0, tiled=True)


def arrival_order(n):
    table = []
    for f in range(n):
        inward = 1 if f < n // 2 else -1
        order = []
        for d in range(1, n):
            for s in (f + inward * d, f - inward * d):
                if 0 <= s < n:
                    order.append(s)
        table.append(order)
    return table


def kernel(
    n,
    tok_hbm, up_hbm, down_hbm, gain_ref, shift_ref,
    out_ref,
    tok, U, Dn, acc, hid, part, half_in, pair, pair_in, summed,
    loc_sem, z_send, z_recv, y_send, y_recv, a_send, a_recv, b_send, b_recv, c_send, c_recv,
):
    g, f, t = lax.axis_index("grp"), lax.axis_index("fs"), lax.axis_index("tp")
    core = lax.rem(t, 2)
    other_g = 1 - g
    mate = t + 1 - 2 * core
    across = lax.rem(t + 2, 4)
    rows, width = tok.shape
    depth = U.shape[1]
    hd = depth // 2
    ff = U.shape[2]
    hw = Dn.shape[3]
    half_rows = rows // 2

    table = arrival_order(n)

    def taken(k):
        s = jnp.int32(table[0][k])
        for i in range(1, n):
            s = jnp.where(f == i, table[i][k], s)
        return s

    order = [taken(k) for k in range(n - 1)]

    def own_up(h, sem):
        r = pl.ds(pl.multiple_of(h * hd, hd), hd)
        return pltpu.make_async_copy(up_hbm.at[r, :], U.at[f, r, :], loc_sem.at[sem])

    def own_down(h, sem):
        c = pl.ds(pl.multiple_of(h * hw, hw), hw)
        return pltpu.make_async_copy(down_hbm.at[:, c], Dn.at[f, h], loc_sem.at[sem])

    local = [
        own_up(g, 0),
        pltpu.make_async_copy(tok_hbm, tok, loc_sem.at[1]),
        own_up(other_g, 2),
        own_down(g, 3),
        own_down(other_g, 4),
    ]
    for c in local:
        c.start()

    barrier = pltpu.get_barrier_semaphore()
    for dev in ({"grp": other_g}, {"tp": mate}, {"tp": across}):
        pl.semaphore_signal(barrier, inc=1, device_id=dev, device_id_type=MESH)

    @pl.when(f > 0)
    def _():
        pl.semaphore_signal(barrier, inc=1, device_id={"fs": f - 1}, device_id_type=MESH)

    @pl.when(f < n - 1)
    def _():
        pl.semaphore_signal(barrier, inc=1, device_id={"fs": f + 1}, device_id_type=MESH)

    pl.semaphore_wait(barrier, 3 + (f > 0).astype(jnp.int32) + (f < n - 1).astype(jnp.int32))

    def piece(array, s, h, sub):
        if array == 0:
            m = hd // SUBS
            return U.at[s, pl.ds(pl.multiple_of(h * hd + sub * m, m), m), :]
        m = ff // SUBS
        return Dn.at[s, h, pl.ds(pl.multiple_of(sub * m, m), m), :]

    def z_copy(array, s, sub, way):
        ref = piece(array, s, g, sub)
        return pltpu.make_async_remote_copy(
            src_ref=ref, dst_ref=ref,
            send_sem=z_send.at[array, s, sub, way], recv_sem=z_recv.at[array, s, sub],
            device_id={"fs": f + (2 * way - 1)}, device_id_type=MESH,
        )

    def y_copy(array, s, h, sub):
        ref = piece(array, s, h, sub)
        return pltpu.make_async_remote_copy(
            src_ref=ref, dst_ref=ref,
            send_sem=y_send.at[array, s, sub], recv_sem=y_recv.at[array, s, sub],
            device_id={"grp": other_g}, device_id_type=MESH,
        )

    def own_sends(array, sub, act):
        @pl.when(f > 0)
        def _():
            act(z_copy(array, f, sub, 0))

        @pl.when(f < n - 1)
        def _():
            act(z_copy(array, f, sub, 1))

    def passes(array, s, sub, act):
        @pl.when((s > f) & (f > 0))
        def _():
            act(z_copy(array, s, sub, 0))

        @pl.when((s < f) & (f < n - 1))
        def _():
            act(z_copy(array, s, sub, 1))

    start = lambda copy: copy.start()
    sent = lambda copy: copy.wait_send()

    def take(array, k, after=None):
        s = order[k]

        def body(sub, carry):
            z_copy(array, s, sub, 0).wait_recv()
            passes(array, s, sub, start)
            y_copy(array, s, g, sub).start()
            if after is not None:
                after(sub)
            return carry

        lax.fori_loop(0, SUBS, body, 0)

    def take_y(array, k):
        s = order[k]

        def body(sub, carry):
            y_copy(array, s, other_g, sub).wait_recv()
            return carry

        lax.fori_loop(0, SUBS, body, 0)

    def up_dot(s, h, first=False):
        r = pl.ds(pl.multiple_of(h * hd, hd), hd)
        kc = pl.ds(pl.multiple_of(s * depth + h * hd, hd), hd)
        tile = ff // 4

        def body(j, carry):
            js = pl.ds(pl.multiple_of(j * tile, tile), tile)
            got = jnp.dot(tok[:, kc], U[s, r, js], preferred_element_type=jnp.float32)
            if first:
                acc[:, js] = got
            else:
                acc[:, js] += got
            return carry

        lax.fori_loop(0, 4, body, 0)

    own_half = pl.ds(pl.multiple_of(core * half_rows, half_rows), half_rows)
    mate_half = pl.ds(pl.multiple_of((1 - core) * half_rows, half_rows), half_rows)

    def a_copy(q):
        return pltpu.make_async_remote_copy(
            src_ref=part.at[q, mate_half, :], dst_ref=half_in.at[q],
            send_sem=a_send.at[q], recv_sem=a_recv.at[q],
            device_id={"tp": mate}, device_id_type=MESH,
        )

    def b_copy(q):
        return pltpu.make_async_remote_copy(
            src_ref=pair.at[q], dst_ref=pair_in.at[q],
            send_sem=b_send.at[q], recv_sem=b_recv.at[q],
            device_id={"tp": across}, device_id_type=MESH,
        )

    def c_copy(q):
        ref = summed.at[q, own_half, :]
        return pltpu.make_async_remote_copy(
            src_ref=ref, dst_ref=ref,
            send_sem=c_send.at[q], recv_sem=c_recv.at[q],
            device_id={"tp": mate}, device_id_type=MESH,
        )

    def down_dot(s, h):
        q = s * 2 + h
        tile = rows // 3

        def body(i, carry):
            r = pl.ds(pl.multiple_of(i * tile, tile), tile)
            part[q, r, :] = jnp.dot(
                hid[r, :], Dn[s, h], preferred_element_type=jnp.float32
            ).astype(jnp.bfloat16)
            return carry

        lax.fori_loop(0, 3, body, 0)
        a_copy(q).start()

    def chip_sum(q):
        a_copy(q).wait_recv()
        pair[q] = (
            part[q, own_half, :].astype(jnp.float32) + half_in[q].astype(jnp.float32)
        ).astype(jnp.bfloat16)
        b_copy(q).start()

    def full_sum(q):
        b_copy(q).wait_recv()
        summed[q, own_half, :] = pair[q].astype(jnp.float32) + pair_in[q].astype(jnp.float32)
        c_copy(q).start()

    local[0].wait()
    lax.fori_loop(0, SUBS, lambda sub, c: (own_sends(0, sub, start), c)[1], 0)
    for c in local[1:]:
        c.wait()
    up_dot(f, 0, first=True)
    up_dot(f, 1)
    for k in range(n - 1):
        after = None
        if k == 1:
            after = lambda sub: own_sends(1, sub, start)
        take(0, k, after)
        up_dot(order[k], g)
        if k > 0:
            take_y(0, k - 1)
            up_dot(order[k - 1], other_g)
    take(1, 0)
    take_y(0, n - 2)
    up_dot(order[n - 2], other_g)

    def activate(i, carry):
        m = rows // 12
        r = pl.ds(pl.multiple_of(i * m, m), m)
        hid[r, :] = jnp.square(jnp.maximum(acc[r, :], 0.0)).astype(jnp.bfloat16)
        return carry

    lax.fori_loop(0, 12, activate, 0)

    done = []

    def block(s, h):
        down_dot(s, h)
        done.append(s * 2 + h)
        if len(done) > 1:
            chip_sum(done[-2])
        if len(done) > 2:
            full_sum(done[-3])

    block(f, g)
    block(f, other_g)
    block(order[0], g)
    for k in range(1, n - 1):
        take(1, k)
        block(order[k], g)
        take_y(1, k - 1)
        block(order[k - 1], other_g)
    take_y(1, n - 2)
    block(order[n - 2], other_g)
    chip_sum(done[-1])
    full_sum(done[-2])
    full_sum(done[-1])
    for q in range(2 * n):
        pltpu.make_async_remote_copy(
            src_ref=summed.at[q, mate_half, :], dst_ref=summed.at[q, mate_half, :],
            send_sem=c_send.at[q], recv_sem=c_recv.at[q],
            device_id={"tp": mate}, device_id_type=MESH,
        ).wait_recv()

    def norm(i, carry):
        m = 16
        r = pl.ds(pl.multiple_of(i * m, m), m)
        total = jnp.concatenate([summed[q, r, :] for q in range(2 * n)], axis=-1)
        out_ref[r, :] = layer_normed(tok[r, :], total, gain_ref[...], shift_ref[...])
        return carry

    lax.fori_loop(0, rows // 16, norm, 0)

    def drain(sub, carry):
        for array in range(2):
            own_sends(array, sub, sent)
            for k in range(n - 1):
                passes(array, order[k], sub, sent)
                y_copy(array, order[k], g, sub).wait_send()
        return carry

    lax.fori_loop(0, SUBS, drain, 0)
    for q in range(2 * n):
        a_copy(q).wait_send()
        b_copy(q).wait_send()
        c_copy(q).wait_send()


def direct(n, tokens, up_weight, down_weight, norm_gain, norm_shift):
    rows, width = tokens.shape
    depth, ff = up_weight.shape
    hw = down_weight.shape[1] // 2
    blocks = 2 * n
    bf16, f32 = jnp.bfloat16, jnp.float32
    dma = pltpu.SemaphoreType.DMA
    anywhere = pl.BlockSpec(memory_space=pl.ANY)
    vmem = pl.BlockSpec(memory_space=pltpu.VMEM)
    return pl.pallas_call(
        functools.partial(kernel, n),
        out_shape=jax.ShapeDtypeStruct((rows, width), bf16),
        in_specs=[anywhere, anywhere, anywhere, vmem, vmem],
        out_specs=vmem,
        scratch_shapes=[
            pltpu.VMEM((rows, width), bf16),
            pltpu.VMEM((n, depth, ff), bf16),
            pltpu.VMEM((n, 2, ff, hw), bf16),
            pltpu.VMEM((rows, ff), f32),
            pltpu.VMEM((rows, ff), bf16),
            pltpu.VMEM((blocks, rows, hw), bf16),
            pltpu.VMEM((blocks, rows // 2, hw), bf16),
            pltpu.VMEM((blocks, rows // 2, hw), bf16),
            pltpu.VMEM((blocks, rows // 2, hw), bf16),
            pltpu.VMEM((blocks, rows, hw), f32),
            dma((5,)),
            dma((2, n, SUBS, 2)),
            dma((2, n, SUBS)),
            dma((2, n, SUBS)),
            dma((2, n, SUBS)),
            dma((blocks,)), dma((blocks,)),
            dma((blocks,)), dma((blocks,)),
            dma((blocks,)), dma((blocks,)),
        ],
        compiler_params=pltpu.CompilerParams(
            collective_id=0, has_side_effects=True, vmem_limit_bytes=60 * 1024 * 1024
        ),
    )(tokens, up_weight, down_weight, norm_gain[None, :], norm_shift[None, :])


def solution(mesh):
    placed = (P(("grp", "fs"), None), P("fs", "tp"), P("tp", "fs"), P(), P())
    n = mesh.shape["fs"]
    fits = mesh.shape["grp"] == 2 and mesh.shape["tp"] == 4 and n == 4
    return jax.shard_map(
        functools.partial(direct, n) if fits else general,
        mesh=mesh, in_specs=placed, out_specs=P(("grp", "fs"), None), check_vma=False,
    )
```

```python
import functools

import jax
import jax.numpy as jnp
from jax import lax
from jax.experimental import pallas as pl
from jax.experimental.pallas import tpu as pltpu
from jax.sharding import PartitionSpec as P

MESH = pl.DeviceIdType.MESH
RESIDUAL_SCALE = 2.0**0.25
NORM_EPS = 1e-05
SUBS = 4


def layer_normed(residual, summed, norm_gain, norm_shift):
    pre_norm = RESIDUAL_SCALE * residual.astype(jnp.float32) + summed
    centre = jnp.mean(pre_norm, axis=-1, keepdims=True)
    centered = pre_norm - centre
    variance = jnp.mean(centered * centered, axis=-1, keepdims=True)
    return (centered * lax.rsqrt(variance + NORM_EPS) * norm_gain + norm_shift).astype(jnp.bfloat16)


def general(tokens, up_weight, down_weight, norm_gain, norm_shift):
    upward = jnp.dot(
        tokens,
        lax.all_gather(up_weight, "fs", axis=0, tiled=True),
        preferred_element_type=jnp.float32,
    )
    down_full = lax.all_gather(down_weight, "fs", axis=1, tiled=True)
    hidden = jnp.square(jax.nn.relu(upward)).astype(jnp.bfloat16)
    share = tokens.shape[0] // lax.axis_size("tp")
    summed = lax.psum_scatter(
        jnp.dot(hidden, down_full, preferred_element_type=jnp.float32).astype(jnp.bfloat16),
        "tp",
        scatter_dimension=0,
        tiled=True,
    ).astype(jnp.float32)
    own_start = lax.axis_index("tp") * share
    own_tokens = lax.dynamic_slice_in_dim(tokens, own_start, share, 0)
    normed = layer_normed(own_tokens, summed, norm_gain, norm_shift)
    return lax.all_gather(normed, "tp", axis=0, tiled=True)


def kernel(
    n,
    tok_hbm, up_hbm, down_hbm, gain_ref, shift_ref,
    out_ref,
    tok, U, Dn, acc, hid, part, half_in, pair, pair_in, summed, quarter,
    loc_sem, z_send, z_recv, y_send, y_recv, t_send, t_recv, g_send, g_recv,
    a_send, a_recv, b_send, b_recv, c_send, c_recv, e_send, e_recv, h_send, h_recv,
):
    g, f, t = lax.axis_index("grp"), lax.axis_index("fs"), lax.axis_index("tp")
    core, chip = lax.rem(t, 2), t // 2
    other_g = 1 - g
    mate = t + 1 - 2 * core
    across = lax.rem(t + 2, 4)
    pal = f + 1 - 2 * lax.rem(f, 2)
    inner = (f > 0) & (f < n - 1)
    fi, fo = jnp.where(inner, f, pal), jnp.where(inner, pal, f)
    ri, ro = n - 1 - fi, n - 1 - fo
    rows, width = out_ref.shape
    depth, ff, hw = U.shape[1], U.shape[2], Dn.shape[3]
    hd = depth // 2
    hr, qr = rows // 2, rows // 4
    place = core * 2 + chip
    blocks = 2 * n

    def own_up(h, sem):
        r = pl.ds(pl.multiple_of(h * hd, hd), hd)
        return pltpu.make_async_copy(up_hbm.at[r, :], U.at[f, r, :], loc_sem.at[sem])

    def own_down(h, sem):
        c = pl.ds(pl.multiple_of(h * hw, hw), hw)
        return pltpu.make_async_copy(down_hbm.at[:, c], Dn.at[f, h], loc_sem.at[sem])

    local = [
        own_up(g, 0),
        pltpu.make_async_copy(tok_hbm, tok.at[pl.ds(0, rows), :], loc_sem.at[1]),
        own_up(other_g, 2),
        own_down(g, 3),
        own_down(other_g, 4),
    ]
    for c in local:
        c.start()

    barrier = pltpu.get_barrier_semaphore()
    peers = [lax.rem(t + d, 4) for d in (1, 2, 3)]
    for dev in [{"grp": other_g}, {"fs": pal}] + [{"tp": p} for p in peers]:
        pl.semaphore_signal(barrier, inc=1, device_id=dev, device_id_type=MESH)

    @pl.when(inner)
    def _():
        pl.semaphore_signal(barrier, inc=1, device_id={"fs": n - 1 - f}, device_id_type=MESH)

    pl.semaphore_wait(barrier, 5 + inner.astype(jnp.int32))

    def remote(src, dst, send, recv, dev):
        return pltpu.make_async_remote_copy(
            src_ref=src, dst_ref=dst, send_sem=send, recv_sem=recv,
            device_id=dev, device_id_type=MESH,
        )

    def subs(body):
        def step(sub, carry):
            body(sub)
            return carry

        lax.fori_loop(0, SUBS, step, 0)

    def piece(array, s, h, sub):
        if array == 0:
            m = hd // SUBS
            return U.at[s, pl.ds(pl.multiple_of(h * hd + sub * m, m), m), :]
        m = ff // SUBS
        return Dn.at[s, h, pl.ds(pl.multiple_of(sub * m, m), m), :]

    def to_pal(array, s, h, sub):
        ref = piece(array, s, h, sub)
        return remote(ref, ref, z_send.at[array, s, h, sub], z_recv.at[array, s, h, sub], {"fs": pal})

    def to_inner(array, s, sub):
        ref = piece(array, s, g, sub)
        return remote(ref, ref, z_send.at[array, s, g, sub], z_recv.at[array, s, g, sub], {"fs": n - 1 - f})

    def to_grp(array, s, h, sub):
        ref = piece(array, s, h, sub)
        return remote(ref, ref, y_send.at[array, s, sub], y_recv.at[array, s, sub], {"grp": other_g})

    def t_copy():
        r = pl.ds(pl.multiple_of(place * qr, qr), qr)
        d = pl.ds(pl.multiple_of(rows + place * qr, qr), qr)
        return remote(tok.at[r, :], tok.at[d, :], t_send, t_recv, {"fs": pal})

    def g_copy(d):
        r = pl.ds(pl.multiple_of(rows + place * qr, qr), qr)
        return remote(tok.at[r, :], tok.at[r, :], g_send.at[d], g_recv.at[d], {"tp": peers[d]})

    own_half = pl.ds(pl.multiple_of(core * hr, hr), hr)
    mate_half = pl.ds(pl.multiple_of((1 - core) * hr, hr), hr)

    def a_copy(q):
        return remote(part.at[q, 1 - core], half_in.at[q], a_send.at[q], a_recv.at[q], {"tp": mate})

    def b_copies(q):
        away = pl.ds(pl.multiple_of(hr + (1 - chip) * qr, qr), qr)
        return [
            remote(pair.at[q, pl.ds(0, hr), :], pair_in.at[q, pl.ds(0, hr), :],
                   b_send.at[0, q], b_recv.at[0, q], {"tp": across}),
            remote(pair.at[q, away, :], pair_in.at[q, pl.ds(hr, qr), :],
                   b_send.at[1, q], b_recv.at[1, q], {"tp": across}),
        ]

    def c_copy(q, r):
        ref = summed.at[q, r, :]
        return remote(ref, ref, c_send.at[q], c_recv.at[q], {"tp": mate})

    def e_copy(q):
        d = pl.ds(pl.multiple_of(place * qr, qr), qr)
        return remote(quarter.at[q], half_in.at[q, d, :], e_send.at[q], e_recv.at[q], {"fs": pal})

    def h_copy(q, d):
        ref = half_in.at[q, pl.ds(pl.multiple_of(place * qr, qr), qr), :]
        return remote(ref, ref, h_send.at[d, q], h_recv.at[d, q], {"tp": peers[d]})

    sequence = [
        (fi, g), (fi, other_g), (ri, g), (fo, g), (ri, other_g), (ro, g), (fo, other_g), (ro, other_g)
    ]
    sequence = [s * 2 + h for s, h in sequence]

    def normed(read):
        def norm(i, carry):
            m = 16
            r = pl.ds(pl.multiple_of(i * m, m), m)
            total = jnp.concatenate([read(q, r) for q in range(blocks)], axis=-1)
            out_ref[r, :] = layer_normed(tok[r, :], total, gain_ref[...], shift_ref[...])
            return carry

        lax.fori_loop(0, rows // 16, norm, 0)

    @pl.when(jnp.logical_not(inner))
    def _():
        local[0].wait()
        subs(lambda sub: to_pal(0, f, g, sub).start())
        local[1].wait()
        t_copy().start()
        local[2].wait()
        subs(lambda sub: to_pal(0, f, other_g, sub).start())
        local[3].wait()
        subs(lambda sub: to_pal(1, f, g, sub).start())
        local[4].wait()
        subs(lambda sub: to_pal(1, f, other_g, sub).start())
        for q in sequence:
            e_copy(q).wait_recv()
            for d in range(3):
                h_copy(q, d).start()
        for q in sequence:
            for d in range(3):
                h_copy(q, d).wait_recv()
        normed(lambda q, r: half_in[q, r, :].astype(jnp.float32))

        def drain(sub):
            for array in range(2):
                to_pal(array, f, g, sub).wait_send()
                to_pal(array, f, other_g, sub).wait_send()

        subs(drain)
        t_copy().wait_send()
        for q in range(blocks):
            for d in range(3):
                h_copy(q, d).wait_send()

    @pl.when(inner)
    def _():
        def up_dot(s, h, first=False):
            r = pl.ds(pl.multiple_of(h * hd, hd), hd)
            kc = pl.ds(pl.multiple_of(s * depth + h * hd, hd), hd)
            tile = ff // 4

            def body(j, carry):
                js = pl.ds(pl.multiple_of(j * tile, tile), tile)
                got = jnp.dot(tok[pl.ds(0, rows), kc], U[s, r, js], preferred_element_type=jnp.float32)
                if first:
                    acc[:, js] = got
                else:
                    acc[:, js] += got
                return carry

            lax.fori_loop(0, 4, body, 0)

        def activated(x):
            return jnp.square(jnp.maximum(x, 0.0)).astype(jnp.bfloat16)

        def activate(i, carry):
            m = rows // 12
            r = pl.ds(pl.multiple_of(i * m, m), m)
            hid[r, :] = activated(acc[r, :])
            return carry

        def outer_up(i, carry):
            tile = ff // 4
            r = pl.ds(pl.multiple_of(rows + (i // 4) * hr, hr), hr)
            js = pl.ds(pl.multiple_of(lax.rem(i, 4) * tile, tile), tile)
            got = jnp.dot(tok[r, pl.ds(0, depth)], U[0, :, js], preferred_element_type=jnp.float32)
            for s in range(1, n):
                got += jnp.dot(
                    tok[r, pl.ds(s * depth, depth)], U[s, :, js], preferred_element_type=jnp.float32
                )
            hid[r, js] = activated(got)
            return carry

        def down_dot(q):
            s, h = q // 2, lax.rem(q, 2)

            def body(i, carry):
                r = pl.ds(pl.multiple_of(i * hr, hr), hr)
                d = pl.ds(pl.multiple_of((i // 2) * hr, hr), hr)
                part[q, lax.rem(i, 2), d, :] = jnp.dot(
                    hid[r, :], Dn[s, h], preferred_element_type=jnp.float32
                ).astype(jnp.bfloat16)
                return carry

            lax.fori_loop(0, 4, body, 0)
            a_copy(q).start()

        def chip_sum(q):
            a_copy(q).wait_recv()
            pair[q] = (
                part[q, core].astype(jnp.float32) + half_in[q].astype(jnp.float32)
            ).astype(jnp.bfloat16)
            for c in b_copies(q):
                c.start()

        def full_sum(q):
            for c in b_copies(q):
                c.wait_recv()
            keep = pl.ds(pl.multiple_of(hr + chip * qr, qr), qr)
            summed[q, own_half, :] = (
                pair[q, pl.ds(0, hr), :].astype(jnp.float32) + pair_in[q, pl.ds(0, hr), :].astype(jnp.float32)
            )
            c_copy(q, own_half).start()
            quarter[q] = (
                pair[q, keep, :].astype(jnp.float32) + pair_in[q, pl.ds(hr, qr), :].astype(jnp.float32)
            ).astype(jnp.bfloat16)
            e_copy(q).start()

        def take_r(array, s):
            def body(sub):
                to_inner(array, s, sub).wait_recv()
                to_grp(array, s, g, sub).start()

            subs(body)

        def take_l(array, h, on):
            def body(sub):
                to_pal(array, fo, h, sub).wait_recv()
                if on:
                    to_inner(array, fo, sub).start()

            subs(body)

        def take_y(array, s):
            subs(lambda sub: to_grp(array, s, other_g, sub).wait_recv())

        local[0].wait()
        subs(lambda sub: to_inner(0, f, sub).start())
        for c in local[1:]:
            c.wait()
        up_dot(fi, 0, first=True)
        up_dot(fi, 1)

        def both(sub):
            to_pal(0, fo, g, sub).wait_recv()
            to_inner(0, fo, sub).start()
            to_inner(0, ri, sub).wait_recv()
            to_grp(0, ri, g, sub).start()

        subs(both)
        subs(lambda sub: to_inner(1, f, sub).start())
        up_dot(fo, g)
        up_dot(ri, g)
        t_copy().wait_recv()
        for d in range(3):
            g_copy(d).start()
        take_r(0, ro)
        up_dot(ro, g)
        take_y(0, ri)
        up_dot(ri, other_g)
        take_l(0, other_g, False)
        up_dot(fo, other_g)
        take_r(1, ri)
        take_y(0, ro)
        up_dot(ro, other_g)
        lax.fori_loop(0, 12, activate, 0)
        for d in range(3):
            g_copy(d).wait_recv()
        lax.fori_loop(0, 8, outer_up, 0)

        needs = {
            3: lambda: take_l(1, g, True),
            4: lambda: take_y(1, ri),
            5: lambda: take_r(1, ro),
            6: lambda: take_l(1, other_g, False),
            7: lambda: take_y(1, ro),
        }
        for i, q in enumerate(sequence):
            if i in needs:
                needs[i]()
            down_dot(q)
            if i > 0:
                chip_sum(sequence[i - 1])
            if i > 1:
                full_sum(sequence[i - 2])
        chip_sum(sequence[-1])
        full_sum(sequence[-2])
        full_sum(sequence[-1])
        for q in range(blocks):
            c_copy(q, mate_half).wait_recv()
        normed(lambda q, r: summed[q, r, :])

        def drain(sub):
            for array in range(2):
                to_inner(array, f, sub).wait_send()
                to_inner(array, fo, sub).wait_send()
                to_grp(array, ri, g, sub).wait_send()
                to_grp(array, ro, g, sub).wait_send()

        subs(drain)
        for d in range(3):
            g_copy(d).wait_send()
        for q in range(blocks):
            a_copy(q).wait_send()
            for c in b_copies(q):
                c.wait_send()
            c_copy(q, own_half).wait_send()
            e_copy(q).wait_send()


def direct(n, tokens, up_weight, down_weight, norm_gain, norm_shift):
    rows, width = tokens.shape
    depth, ff = up_weight.shape
    hw = down_weight.shape[1] // 2
    blocks = 2 * n
    bf16, f32 = jnp.bfloat16, jnp.float32
    dma = pltpu.SemaphoreType.DMA
    anywhere = pl.BlockSpec(memory_space=pl.ANY)
    vmem = pl.BlockSpec(memory_space=pltpu.VMEM)
    return pl.pallas_call(
        functools.partial(kernel, n),
        out_shape=jax.ShapeDtypeStruct((rows, width), bf16),
        in_specs=[anywhere, anywhere, anywhere, vmem, vmem],
        out_specs=vmem,
        scratch_shapes=[
            pltpu.VMEM((2 * rows, width), bf16),
            pltpu.VMEM((n, depth, ff), bf16),
            pltpu.VMEM((n, 2, ff, hw), bf16),
            pltpu.VMEM((rows, ff), f32),
            pltpu.VMEM((2 * rows, ff), bf16),
            pltpu.VMEM((blocks, 2, rows, hw), bf16),
            pltpu.VMEM((blocks, rows, hw), bf16),
            pltpu.VMEM((blocks, rows, hw), bf16),
            pltpu.VMEM((blocks, 3 * rows // 4, hw), bf16),
            pltpu.VMEM((blocks, rows, hw), f32),
            pltpu.VMEM((blocks, rows // 4, hw), bf16),
            dma((5,)),
            dma((2, n, 2, SUBS)), dma((2, n, 2, SUBS)),
            dma((2, n, SUBS)), dma((2, n, SUBS)),
            dma, dma,
            dma((3,)), dma((3,)),
            dma((blocks,)), dma((blocks,)),
            dma((2, blocks)), dma((2, blocks)),
            dma((blocks,)), dma((blocks,)),
            dma((blocks,)), dma((blocks,)),
            dma((3, blocks)), dma((3, blocks)),
        ],
        compiler_params=pltpu.CompilerParams(
            collective_id=0, has_side_effects=True, vmem_limit_bytes=67043328
        ),
    )(tokens, up_weight, down_weight, norm_gain[None, :], norm_shift[None, :])


def solution(mesh):
    placed = (P(("grp", "fs"), None), P("fs", "tp"), P("tp", "fs"), P(), P())
    n = mesh.shape["fs"]
    fits = mesh.shape["grp"] == 2 and mesh.shape["tp"] == 4 and n == 4
    return jax.shard_map(
        functools.partial(direct, n) if fits else general,
        mesh=mesh, in_specs=placed, out_specs=P(("grp", "fs"), None), check_vma=False,
    )
```

```python
import functools

import jax
import jax.numpy as jnp
from jax import lax
from jax.experimental import pallas as pl
from jax.experimental.pallas import tpu as pltpu
from jax.sharding import PartitionSpec as P

MESH = pl.DeviceIdType.MESH
RESIDUAL_SCALE = 2.0**0.25
NORM_EPS = 1e-05
SUBS = 4


def layer_normed(residual, summed, norm_gain, norm_shift):
    pre_norm = RESIDUAL_SCALE * residual.astype(jnp.float32) + summed
    centre = jnp.mean(pre_norm, axis=-1, keepdims=True)
    centered = pre_norm - centre
    variance = jnp.mean(centered * centered, axis=-1, keepdims=True)
    return (centered * lax.rsqrt(variance + NORM_EPS) * norm_gain + norm_shift).astype(jnp.bfloat16)


def general(tokens, up_weight, down_weight, norm_gain, norm_shift):
    upward = jnp.dot(
        tokens,
        lax.all_gather(up_weight, "fs", axis=0, tiled=True),
        preferred_element_type=jnp.float32,
    )
    down_full = lax.all_gather(down_weight, "fs", axis=1, tiled=True)
    hidden = jnp.square(jax.nn.relu(upward)).astype(jnp.bfloat16)
    share = tokens.shape[0] // lax.axis_size("tp")
    summed = lax.psum_scatter(
        jnp.dot(hidden, down_full, preferred_element_type=jnp.float32).astype(jnp.bfloat16),
        "tp",
        scatter_dimension=0,
        tiled=True,
    ).astype(jnp.float32)
    own_start = lax.axis_index("tp") * share
    own_tokens = lax.dynamic_slice_in_dim(tokens, own_start, share, 0)
    normed = layer_normed(own_tokens, summed, norm_gain, norm_shift)
    return lax.all_gather(normed, "tp", axis=0, tiled=True)


def kernel(
    n,
    tok_hbm, up_hbm, down_hbm, gain_ref, shift_ref,
    out_ref,
    tok, U, Dn, acc, hid, part, half_in, pair, pair_in, summed,
    loc_sem, z_send, z_recv, y_send, y_recv, t_send, t_recv, g_send, g_recv,
    a_send, a_recv, b_send, b_recv, c_send, c_recv, e_send, e_recv,
):
    g, f, t = lax.axis_index("grp"), lax.axis_index("fs"), lax.axis_index("tp")
    core, chip = lax.rem(t, 2), t // 2
    other_g = 1 - g
    mate = t + 1 - 2 * core
    across = lax.rem(t + 2, 4)
    pal = f + 1 - 2 * lax.rem(f, 2)
    inner = (f > 0) & (f < n - 1)
    fi, fo = jnp.where(inner, f, pal), jnp.where(inner, pal, f)
    ri, ro = n - 1 - fi, n - 1 - fo
    rows, width = out_ref.shape
    depth, ff, hw = U.shape[1], U.shape[2], Dn.shape[3]
    hd = depth // 2
    hr, qr = rows // 2, rows // 4
    place = core * 2 + chip
    blocks = 2 * n

    def own_up(h, sem):
        r = pl.ds(pl.multiple_of(h * hd, hd), hd)
        return pltpu.make_async_copy(up_hbm.at[r, :], U.at[f, r, :], loc_sem.at[sem])

    def own_down(h, sem):
        c = pl.ds(pl.multiple_of(h * hw, hw), hw)
        return pltpu.make_async_copy(down_hbm.at[:, c], Dn.at[f, h], loc_sem.at[sem])

    local = [
        own_up(g, 0),
        pltpu.make_async_copy(tok_hbm, tok.at[pl.ds(0, rows), :], loc_sem.at[1]),
        own_up(other_g, 2),
        own_down(g, 3),
        own_down(other_g, 4),
    ]
    for c in local:
        c.start()

    barrier = pltpu.get_barrier_semaphore()
    peers = [lax.rem(t + d, 4) for d in (1, 2, 3)]
    for dev in [{"grp": other_g}, {"fs": pal}] + [{"tp": p} for p in peers]:
        pl.semaphore_signal(barrier, inc=1, device_id=dev, device_id_type=MESH)

    @pl.when(inner)
    def _():
        pl.semaphore_signal(barrier, inc=1, device_id={"fs": n - 1 - f}, device_id_type=MESH)

    pl.semaphore_wait(barrier, 5 + inner.astype(jnp.int32))

    def remote(src, dst, send, recv, dev):
        return pltpu.make_async_remote_copy(
            src_ref=src, dst_ref=dst, send_sem=send, recv_sem=recv,
            device_id=dev, device_id_type=MESH,
        )

    def subs(body):
        def step(sub, carry):
            body(sub)
            return carry

        lax.fori_loop(0, SUBS, step, 0)

    def piece(array, s, h, sub):
        if array == 0:
            m = hd // SUBS
            return U.at[s, pl.ds(pl.multiple_of(h * hd + sub * m, m), m), :]
        m = ff // SUBS
        return Dn.at[s, h, pl.ds(pl.multiple_of(sub * m, m), m), :]

    def to_pal(array, s, h, sub):
        ref = piece(array, s, h, sub)
        return remote(ref, ref, z_send.at[array, s, h, sub], z_recv.at[array, s, h, sub], {"fs": pal})

    def to_inner(array, s, sub):
        ref = piece(array, s, g, sub)
        return remote(ref, ref, z_send.at[array, s, g, sub], z_recv.at[array, s, g, sub], {"fs": n - 1 - f})

    def to_grp(array, s, h, sub):
        ref = piece(array, s, h, sub)
        return remote(ref, ref, y_send.at[array, s, sub], y_recv.at[array, s, sub], {"grp": other_g})

    def t_copy():
        r = pl.ds(pl.multiple_of(place * qr, qr), qr)
        d = pl.ds(pl.multiple_of(rows + place * qr, qr), qr)
        return remote(tok.at[r, :], tok.at[d, :], t_send, t_recv, {"fs": pal})

    def g_copy(d):
        r = pl.ds(pl.multiple_of(rows + place * qr, qr), qr)
        return remote(tok.at[r, :], tok.at[r, :], g_send.at[d], g_recv.at[d], {"tp": peers[d]})

    own_half = pl.ds(pl.multiple_of(core * hr, hr), hr)
    mate_half = pl.ds(pl.multiple_of((1 - core) * hr, hr), hr)

    def a_copy(q):
        return remote(part.at[q, 1 - core], half_in.at[q], a_send.at[q], a_recv.at[q], {"tp": mate})

    def b_copy(q):
        return remote(
            pair.at[q, pl.ds(0, hr), :], pair_in.at[q], b_send.at[q], b_recv.at[q], {"tp": across}
        )

    def c_copy(q, r):
        ref = summed.at[q, r, :]
        return remote(ref, ref, c_send.at[q], c_recv.at[q], {"tp": mate})

    def e_copy(q):
        return remote(
            pair.at[q, pl.ds(hr, hr), :], pair.at[q, pl.ds(0, hr), :], e_send.at[q], e_recv.at[q], {"fs": pal}
        )

    def full_sum(q):
        b_copy(q).wait_recv()
        summed[q, own_half, :] = (
            pair[q, pl.ds(0, hr), :].astype(jnp.float32) + pair_in[q].astype(jnp.float32)
        )
        c_copy(q, own_half).start()

    def normed_sums():
        for q in range(blocks):
            c_copy(q, mate_half).wait_recv()
        normed(lambda q, r: summed[q, r, :])

    sequence = [
        (fi, g), (fi, other_g), (ri, g), (fo, g), (ri, other_g), (ro, g), (fo, other_g), (ro, other_g)
    ]
    sequence = [s * 2 + h for s, h in sequence]

    def normed(read):
        def norm(i, carry):
            m = 64
            r = pl.ds(pl.multiple_of(i * m, m), m)
            total = jnp.concatenate([read(q, r) for q in range(blocks)], axis=-1)
            out_ref[r, :] = layer_normed(tok[r, :], total, gain_ref[...], shift_ref[...])
            return carry

        lax.fori_loop(0, rows // 64, norm, 0)

    @pl.when(jnp.logical_not(inner))
    def _():
        local[1].wait()
        t_copy().start()
        local[0].wait()
        subs(lambda sub: to_pal(0, f, g, sub).start())
        local[2].wait()
        subs(lambda sub: to_pal(0, f, other_g, sub).start())
        local[3].wait()
        subs(lambda sub: to_pal(1, f, g, sub).start())
        local[4].wait()
        for sub in range(SUBS - 1):
            to_pal(1, f, other_g, sub).start()
        for i, q in enumerate(sequence):
            e_copy(q).wait_recv()
            b_copy(q).start()
            if i > 0:
                full_sum(sequence[i - 1])
        full_sum(sequence[-1])
        normed_sums()

        def drain(sub):
            for array in range(2):
                to_pal(array, f, g, sub).wait_send()
            to_pal(0, f, other_g, sub).wait_send()

        subs(drain)
        for sub in range(SUBS - 1):
            to_pal(1, f, other_g, sub).wait_send()
        t_copy().wait_send()
        for q in range(blocks):
            b_copy(q).wait_send()
            c_copy(q, own_half).wait_send()

    @pl.when(inner)
    def _():
        def up_dot(s, h, first=False):
            r = pl.ds(pl.multiple_of(h * hd, hd), hd)
            kc = pl.ds(pl.multiple_of(s * depth + h * hd, hd), hd)
            tile = ff // 4

            def body(j, carry):
                js = pl.ds(pl.multiple_of(j * tile, tile), tile)
                got = jnp.dot(tok[pl.ds(0, rows), kc], U[s, r, js], preferred_element_type=jnp.float32)
                if first:
                    acc[:, js] = got
                else:
                    acc[:, js] += got
                return carry

            lax.fori_loop(0, 4, body, 0)

        def activated(x):
            return jnp.square(jnp.maximum(x, 0.0)).astype(jnp.bfloat16)

        def activate(i, carry):
            m = rows // 12
            r = pl.ds(pl.multiple_of(i * m, m), m)
            hid[r, :] = activated(acc[r, :])
            return carry

        def outer_up(i, carry):
            tile = ff // 4
            r = pl.ds(pl.multiple_of(rows + (i // 4) * hr, hr), hr)
            js = pl.ds(pl.multiple_of(lax.rem(i, 4) * tile, tile), tile)
            got = jnp.dot(tok[r, pl.ds(0, depth)], U[0, :, js], preferred_element_type=jnp.float32)
            for s in range(1, n):
                got += jnp.dot(
                    tok[r, pl.ds(s * depth, depth)], U[s, :, js], preferred_element_type=jnp.float32
                )
            hid[r, js] = activated(got)
            return carry

        def down_dot(q):
            s, h = q // 2, lax.rem(q, 2)

            def body(i, carry):
                r = pl.ds(pl.multiple_of(i * hr, hr), hr)
                d = pl.ds(pl.multiple_of((i // 2) * hr, hr), hr)
                part[q, lax.rem(i, 2), d, :] = jnp.dot(
                    hid[r, :], Dn[s, h], preferred_element_type=jnp.float32
                ).astype(jnp.bfloat16)
                return carry

            lax.fori_loop(0, 4, body, 0)
            a_copy(q).start()

        def chip_sum(q):
            a_copy(q).wait_recv()
            pair[q] = (
                part[q, core].astype(jnp.float32) + half_in[q].astype(jnp.float32)
            ).astype(jnp.bfloat16)
            b_copy(q).start()
            e_copy(q).start()

        def take_r(array, s):
            def body(sub):
                to_inner(array, s, sub).wait_recv()
                to_grp(array, s, g, sub).start()

            subs(body)

        def take_l(array, h, on):
            def body(sub):
                to_pal(array, fo, h, sub).wait_recv()
                if on:
                    to_inner(array, fo, sub).start()

            subs(body)

        def take_y(array, s):
            subs(lambda sub: to_grp(array, s, other_g, sub).wait_recv())

        local[0].wait()
        subs(lambda sub: to_inner(0, f, sub).start())
        for c in local[1:]:
            c.wait()
        up_dot(fi, 0, first=True)
        up_dot(fi, 1)

        take_r(0, ri)
        t_copy().wait_recv()
        for d in range(3):
            g_copy(d).start()
        up_dot(ri, g)
        take_l(0, g, True)
        subs(lambda sub: to_inner(1, f, sub).start())
        up_dot(fo, g)
        take_r(0, ro)
        up_dot(ro, g)
        take_y(0, ri)
        up_dot(ri, other_g)
        take_l(0, other_g, False)
        up_dot(fo, other_g)
        take_r(1, ri)
        take_y(0, ro)
        up_dot(ro, other_g)
        lax.fori_loop(0, 12, activate, 0)
        for d in range(3):
            g_copy(d).wait_recv()
        lax.fori_loop(0, 8, outer_up, 0)

        def take_last():
            for sub in range(SUBS - 1):
                to_pal(1, fo, other_g, sub).wait_recv()
            to_grp(1, fo, other_g, SUBS - 1).wait_recv()

        needs = {
            3: lambda: (take_l(1, g, True), to_grp(1, fo, g, SUBS - 1).start()),
            4: lambda: take_y(1, ri),
            5: lambda: take_r(1, ro),
            6: take_last,
            7: lambda: take_y(1, ro),
        }
        for i, q in enumerate(sequence):
            if i in needs:
                needs[i]()
            down_dot(q)
            if i > 0:
                chip_sum(sequence[i - 1])
            if i > 1:
                full_sum(sequence[i - 2])
        chip_sum(sequence[-1])
        full_sum(sequence[-2])
        full_sum(sequence[-1])
        normed_sums()

        def drain(sub):
            for array in range(2):
                to_inner(array, f, sub).wait_send()
                to_inner(array, fo, sub).wait_send()
                to_grp(array, ri, g, sub).wait_send()
                to_grp(array, ro, g, sub).wait_send()

        subs(drain)
        to_grp(1, fo, g, SUBS - 1).wait_send()
        for d in range(3):
            g_copy(d).wait_send()
        for q in range(blocks):
            a_copy(q).wait_send()
            b_copy(q).wait_send()
            c_copy(q, own_half).wait_send()
            e_copy(q).wait_send()


def direct(n, tokens, up_weight, down_weight, norm_gain, norm_shift):
    rows, width = tokens.shape
    depth, ff = up_weight.shape
    hw = down_weight.shape[1] // 2
    blocks = 2 * n
    bf16, f32 = jnp.bfloat16, jnp.float32
    dma = pltpu.SemaphoreType.DMA
    anywhere = pl.BlockSpec(memory_space=pl.ANY)
    vmem = pl.BlockSpec(memory_space=pltpu.VMEM)
    return pl.pallas_call(
        functools.partial(kernel, n),
        out_shape=jax.ShapeDtypeStruct((rows, width), bf16),
        in_specs=[anywhere, anywhere, anywhere, vmem, vmem],
        out_specs=vmem,
        scratch_shapes=[
            pltpu.VMEM((2 * rows, width), bf16),
            pltpu.VMEM((n, depth, ff), bf16),
            pltpu.VMEM((n, 2, ff, hw), bf16),
            pltpu.VMEM((rows, ff), f32),
            pltpu.VMEM((2 * rows, ff), bf16),
            pltpu.VMEM((blocks, 2, rows, hw), bf16),
            pltpu.VMEM((blocks, rows, hw), bf16),
            pltpu.VMEM((blocks, rows, hw), bf16),
            pltpu.VMEM((blocks, rows // 2, hw), bf16),
            pltpu.VMEM((blocks, rows, hw), f32),
            dma((5,)),
            dma((2, n, 2, SUBS)), dma((2, n, 2, SUBS)),
            dma((2, n, SUBS)), dma((2, n, SUBS)),
            dma, dma,
            dma((3,)), dma((3,)),
            dma((blocks,)), dma((blocks,)),
            dma((blocks,)), dma((blocks,)),
            dma((blocks,)), dma((blocks,)),
            dma((blocks,)), dma((blocks,)),
        ],
        compiler_params=pltpu.CompilerParams(
            collective_id=0, has_side_effects=True, vmem_limit_bytes=67043328
        ),
    )(tokens, up_weight, down_weight, norm_gain[None, :], norm_shift[None, :])


def solution(mesh):
    placed = (P(("grp", "fs"), None), P("fs", "tp"), P("tp", "fs"), P(), P())
    n = mesh.shape["fs"]
    fits = mesh.shape["grp"] == 2 and mesh.shape["tp"] == 4 and n == 4
    return jax.shard_map(
        functools.partial(direct, n) if fits else general,
        mesh=mesh, in_specs=placed, out_specs=P(("grp", "fs"), None), check_vma=False,
    )
```
